32 devices in a mesh: ep: 16 (over z, y, x), tp: 2 (over core).
Axes of the slice: x: 2, y: 2, z: 4, core: 2. Of those that a mesh axis runs over, the one named last changes fastest.
Arguments:
- tokens: bfloat16 [256, 2048], P('ep'), may hold values from -6 to 6
- recurrent_state: float32 [256, 4, 128, 256], P('ep', 'tp'), may hold values from -6 to 6
- query_weight: bfloat16 [2048, 512], P(None, 'tp'), may hold values from -0.125 to 0.125
- key_weight: bfloat16 [2048, 512], P(None, 'tp'), may hold values from -0.125 to 0.125
- decay_weight: bfloat16 [2048, 512], P(None, 'tp'), may hold values from -0.5 to 0.5
- value_weight: bfloat16 [2048, 1024], P(None, 'tp'), may hold values from -0.125 to 0.125
- gate_weight: bfloat16 [2048, 1024], P(None, 'tp'), may hold values from -0.125 to 0.125
- head_gain: float32 [256], replicated, may hold values from 0.1 to 1.9
- output_weight: bfloat16 [1024, 2048], P('tp'), may hold values from -0.375 to 0.375
- norm_gain: float32 [2, 2048], replicated, may hold values from 0.1 to 1.9
- norm_bias: float32 [2, 2048], replicated, may hold values from -1.8 to 1.8
- group_router: bfloat16 [2048, 4], replicated, may hold values from -0.125 to 0.125
- router_weight: bfloat16 [2048, 32], replicated, may hold values from -0.125 to 0.125
- routes: int32 [256, 2], P('ep'), may hold values from 0 to 31, as said below
- expert_gate: bfloat16 [32, 2048, 256], P(('ep', 'tp')), may hold values from -0.125 to 0.125
- expert_up: bfloat16 [32, 2048, 256], P(('ep', 'tp')), may hold values from -0.125 to 0.125
- expert_down: bfloat16 [32, 256, 2048], P(('ep', 'tp')), may hold values from -1.5 to 1.5
Outputs:
- new_tokens: bfloat16 [256, 2048], P('ep', 'tp')
- new_state: float32 [256, 4, 128, 256], P('ep', 'tp')
The draws below stay inside these ranges and needn't reach their ends.
Inputs may be any that keep to these rules, and one draw needn't show every extreme that they name: `routes`: each row names two different experts of one group (group g holds the experts g * 8 to g * 8 + 7). In the rows of one device each group is named by the same number of rows and no expert by more than 2 rows; some expert is named by exactly 2 rows of every device.
All inputs are finite; a program needn't handle non-finite values.
Results may differ from the reference program's by a relative error of at most 0.01.
Values may be sent and summed in bfloat16 or wider, within the bound.
No kernel may reach another device: no remote copies, remote signals or barrier semaphores. Data moves between devices by JAX's collectives and lax.ppermute only.
A program may use at most 128 MiB of HBM per device.

```python
import jax
import jax.numpy as jnp
from jax import lax

D = 2048
HEADS = 4
DK = 128
DV = 256
EXPERT_FF = 256
GROUPS = 4
TOPK = 2
SEQ_DEV = 16
KW = 512
VW = 1024
EXPERTS = 32
EPG = 8
BATCH = 256
CAP = 2
N_EP = 16
N_TP = 2


def draw_routes(key, part):
    per_group = EXPERTS // GROUPS
    block_keys = jax.random.split(jax.random.fold_in(key, 11), N_EP)

    def permute(subkey):
        return jax.random.permutation(subkey, SEQ_DEV)
    rank_order = jax.vmap(permute)(block_keys).astype(jnp.int32)
    group_id = rank_order % GROUPS
    within_group = rank_order // GROUPS
    offsets = jax.random.randint(jax.random.fold_in(key, 12), (N_EP, GROUPS), 0, per_group).astype(jnp.int32)
    offsets = offsets.at[0, 0].set(0).at[0, GROUPS - 1].set(per_group - 1)
    extra_gap = jax.random.randint(jax.random.fold_in(key, 14), (N_EP, GROUPS), 0, 2).astype(jnp.int32)
    row_offset = jnp.take_along_axis(offsets, group_id, axis=1)
    row_gap = jnp.take_along_axis(extra_gap, group_id, axis=1)
    first_pick = group_id * per_group + (within_group + row_offset) % per_group
    second_pick = group_id * per_group + (within_group + row_offset + 1 + row_gap) % per_group
    flip_bits = jax.random.randint(jax.random.fold_in(key, 13), (N_EP, SEQ_DEV), 0, 2)
    lead_pick = jnp.where(flip_bits == 1, second_pick, first_pick)
    trail_pick = jnp.where(flip_bits == 1, first_pick, second_pick)
    return jnp.stack([lead_pick, trail_pick], axis=-1).reshape(BATCH, 2).astype(jnp.int32)


def level_of(own_key, extent, shards, smallest, largest):
    gain = 1.0
    for position, shards_of in shards:
        steps = jax.random.uniform(jax.random.fold_in(jax.random.fold_in(own_key, 6), position), (shards_of,), jnp.float32, smallest / len(shards), largest / len(shards))
        gain = gain * jnp.repeat(jnp.exp(steps), extent[position] // shards_of).reshape((-1,) + (1,) * (len(extent) - 1 - position))
    return gain


def centred(own_key, extent, width, bound, cuts=(), kind=jnp.bfloat16):
    array = width * jax.random.normal(own_key, extent, jnp.float32)
    if cuts:
        array = array * level_of(own_key, extent, cuts, -0.22, 0.18)
    return jnp.clip(array, -bound, bound).astype(kind)


def setup_inputs(seed: int = 0) -> dict:
    key_list = jax.random.split(jax.random.key(seed), 18)
    return {
        "tokens": centred(key_list[0], (BATCH, D), 1.0, 6.0, ((0, 16),)),
        "recurrent_state": centred(key_list[1], (BATCH, HEADS, DK, DV), 1.0, 6.0, ((0, 16), (1, 2)), jnp.float32),
        "query_weight": centred(key_list[2], (D, KW), D ** -0.5, 0.125, ((1, 2),)),
        "key_weight": centred(key_list[3], (D, KW), D ** -0.5, 0.125, ((1, 2),)),
        "decay_weight": centred(key_list[4], (D, KW), (D // 16) ** -0.5, 0.5, ((1, 2),)),
        "value_weight": centred(key_list[5], (D, VW), D ** -0.5, 0.125, ((1, 2),)),
        "gate_weight": centred(key_list[6], (D, VW), D ** -0.5, 0.125, ((1, 2),)),
        "head_gain": jnp.clip(1.0 + 0.18 * jax.random.normal(key_list[7], (DV,), jnp.float32), 0.1, 1.9),
        "output_weight": centred(key_list[8], (VW, D), (VW // 4) ** -0.5, 0.375, ((0, 2),)),
        "norm_gain": jnp.clip(1.0 + 0.18 * jax.random.normal(key_list[9], (2, D), jnp.float32), 0.1, 1.9),
        "norm_bias": centred(key_list[10], (2, D), 0.3, 1.8, (), jnp.float32),
        "group_router": centred(key_list[11], (D, GROUPS), D ** -0.5, 0.125),
        "router_weight": centred(key_list[12], (D, EXPERTS), D ** -0.5, 0.125),
        "routes": draw_routes(jax.random.fold_in(key_list[17], 71), 0),
        "expert_gate": centred(key_list[14], (EXPERTS, D, EXPERT_FF), D ** -0.5, 0.125, ((0, 32),)),
        "expert_up": centred(key_list[15], (EXPERTS, D, EXPERT_FF), D ** -0.5, 0.125, ((0, 32),)),
        "expert_down": centred(key_list[16], (EXPERTS, EXPERT_FF, D), (EXPERT_FF // 16) ** -0.5, 1.5, ((0, 32),)),
    }


alpha_res = 2.0 ** 0.5
eps_norm = 1e-05

def layer_normed(inputs, gain_row, bias_row):
    centered = inputs - lax.optimization_barrier(jnp.mean(inputs, axis=-1, keepdims=True))
    spread = lax.optimization_barrier(jnp.mean(centered * centered, axis=-1, keepdims=True))
    return centered * lax.rsqrt(spread + eps_norm) * gain_row + bias_row

def rounded_back(values_in):
    return lax.optimization_barrier(values_in.astype(jnp.bfloat16)).astype(jnp.float32)

def reference(tokens, recurrent_state, query_weight, key_weight, decay_weight, value_weight, gate_weight, head_gain, output_weight, norm_gain, norm_bias, group_router, router_weight, routes, expert_gate, expert_up, expert_down):

    def project(weight):
        return jnp.dot(tokens, weight, preferred_element_type=jnp.float32)
    queries = project(query_weight).reshape(BATCH, HEADS, DK) * DK ** (-0.5)
    key_rows = project(key_weight).reshape(BATCH, HEADS, DK)
    value_rows = project(value_weight).reshape(BATCH, HEADS, DV)
    gate_rows = project(gate_weight)
    log_decay = (jax.nn.log_sigmoid(project(decay_weight)) / 16.0).reshape(BATCH, HEADS, DK)
    new_state = jnp.exp(log_decay)[..., None] * recurrent_state + key_rows[..., None] * value_rows[:, :, None, :]
    readout = lax.optimization_barrier(jnp.sum(queries[..., None] * new_state, axis=2))
    norm_scale = lax.rsqrt(lax.optimization_barrier(jnp.mean(readout * readout, axis=-1, keepdims=True)) + eps_norm)
    gated = ((readout * norm_scale * head_gain).reshape(BATCH, VW) * jax.nn.silu(gate_rows)).astype(jnp.bfloat16)
    group_cols = VW // N_TP
    mixed_sum = jnp.zeros((BATCH, D), jnp.float32)
    for part_index in range(N_TP):
        product_part = jnp.dot(gated[:, part_index * group_cols:(part_index + 1) * group_cols], output_weight[part_index * group_cols:(part_index + 1) * group_cols], preferred_element_type=jnp.float32)
        mixed_sum = mixed_sum + rounded_back(product_part)
    hidden = layer_normed(alpha_res * tokens.astype(jnp.float32) + mixed_sum, norm_gain[0], norm_bias[0]).astype(jnp.bfloat16)
    group_logit = jnp.dot(hidden, group_router, preferred_element_type=jnp.float32)
    expert_logit = jnp.dot(hidden, router_weight, preferred_element_type=jnp.float32)
    chosen_group = routes[:, 0] // EPG
    group_hit = chosen_group[:, None] == jnp.arange(GROUPS, dtype=jnp.int32)[None, :]
    own_logit = lax.optimization_barrier(jnp.sum(jnp.where(group_hit, group_logit, 0.0), axis=1, keepdims=True))
    group_share = 1.0 / lax.optimization_barrier(jnp.sum(jnp.exp(group_logit - own_logit), axis=1))
    expert_hit = routes[:, :, None] == jnp.arange(EXPERTS, dtype=jnp.int32)[None, None, :]
    picked = lax.optimization_barrier(jnp.sum(jnp.where(expert_hit, expert_logit[:, None, :], 0.0), axis=2))
    route_weight = group_share[:, None] * jax.nn.sigmoid(picked - picked[:, ::-1])
    flat_routes = routes.reshape(BATCH * TOPK)
    row_limit = N_EP * CAP

    def serve_expert(expert_index):
        hit_index = jnp.nonzero(flat_routes == expert_index, size=row_limit, fill_value=BATCH * TOPK)[0].astype(jnp.int32)
        rows_in = hidden[jnp.minimum(hit_index, BATCH * TOPK - 1) // TOPK]
        gate_part = jnp.dot(rows_in, expert_gate[expert_index], preferred_element_type=jnp.float32)
        up_part = jnp.dot(rows_in, expert_up[expert_index], preferred_element_type=jnp.float32)
        activation = (jax.nn.silu(gate_part) * up_part).astype(jnp.bfloat16)
        combined = jnp.dot(activation, expert_down[expert_index], preferred_element_type=jnp.float32)
        return (hit_index, combined.astype(jnp.bfloat16))
    all_index, all_out = lax.map(serve_expert, jnp.arange(EXPERTS, dtype=jnp.int32))
    expert_out = jnp.zeros((BATCH * TOPK, D), jnp.bfloat16).at[all_index.reshape(-1)].set(all_out.reshape(-1, D), mode='drop')
    routed_sum = lax.optimization_barrier(jnp.sum(route_weight[..., None] * expert_out.reshape(BATCH, TOPK, D).astype(jnp.float32), axis=1))
    new_tokens = layer_normed(alpha_res * hidden.astype(jnp.float32) + routed_sum, norm_gain[1], norm_bias[1]).astype(jnp.bfloat16)
    return (new_tokens, new_state)
```

```python
import jax
import jax.numpy as jnp
from jax import lax
from jax.sharding import PartitionSpec as P

alpha_res = 2.0**0.5
eps_norm = 1e-05


def layer_normed(inputs, gain_row, bias_row):
    centered = inputs - jnp.mean(inputs, axis=-1, keepdims=True)
    spread = jnp.mean(centered * centered, axis=-1, keepdims=True)
    return centered * lax.rsqrt(spread + eps_norm) * gain_row + bias_row


def swapped(values):
    count = lax.axis_size("tp")
    return lax.ppermute(values, "tp", [(i, (i + 1) % count) for i in range(count)])


def on_device(
    tokens,
    recurrent_state,
    query_weight,
    key_weight,
    decay_weight,
    value_weight,
    gate_weight,
    head_gain,
    output_weight,
    norm_gain,
    norm_bias,
    group_router,
    router_weight,
    routes,
    expert_gate,
    expert_up,
    expert_down,
):
    row_count, model_width = tokens.shape
    heads_here = recurrent_state.shape[1]
    key_dim = recurrent_state.shape[2]
    value_dim = recurrent_state.shape[3]

    def project(weight):
        return jnp.dot(tokens, weight, preferred_element_type=jnp.float32)

    queries = project(query_weight).reshape(row_count, heads_here, key_dim) * key_dim ** (-0.5)
    key_rows = project(key_weight).reshape(row_count, heads_here, key_dim)
    value_rows = project(value_weight).reshape(row_count, heads_here, value_dim)
    gate_rows = project(gate_weight)
    decay_rate = jnp.exp(jax.nn.log_sigmoid(project(decay_weight)) / 16.0).reshape(
        row_count, heads_here, key_dim
    )
    readout = (
        jnp.sum((queries * decay_rate)[..., None] * recurrent_state, axis=2)
        + jnp.sum(queries * key_rows, axis=-1, keepdims=True) * value_rows
    )
    norm_scale = lax.rsqrt(jnp.mean(readout * readout, axis=-1, keepdims=True) + eps_norm)
    gated_rows = (
        (readout * norm_scale * head_gain).reshape(row_count, heads_here * value_dim)
        * jax.nn.silu(gate_rows)
    ).astype(jnp.bfloat16)
    partial_value = jnp.dot(gated_rows, output_weight, preferred_element_type=jnp.float32)
    own_part = partial_value.astype(jnp.bfloat16)
    mixed_sum = own_part.astype(jnp.float32) + swapped(own_part).astype(jnp.float32)
    hidden = layer_normed(
        alpha_res * tokens.astype(jnp.float32) + mixed_sum, norm_gain[0], norm_bias[0]
    ).astype(jnp.bfloat16)
    group_count = group_router.shape[1]
    expert_count = router_weight.shape[1]
    per_group = expert_count // group_count
    top_count = routes.shape[1]
    group_logit = jnp.dot(hidden, group_router, preferred_element_type=jnp.float32)
    expert_logit = jnp.dot(hidden, router_weight, preferred_element_type=jnp.float32)
    chosen_group = routes[:, 0] // per_group
    group_hit = chosen_group[:, None] == jnp.arange(group_count, dtype=jnp.int32)[None, :]
    own_logit = jnp.sum(jnp.where(group_hit, group_logit, 0.0), axis=1, keepdims=True)
    group_share = 1.0 / jnp.sum(jnp.exp(group_logit - own_logit), axis=1)
    expert_hit = routes[:, :, None] == jnp.arange(expert_count, dtype=jnp.int32)[None, None, :]
    picked = jnp.sum(jnp.where(expert_hit, expert_logit[:, None, :], 0.0), axis=2)
    route_weight = group_share[:, None] * jax.nn.sigmoid(picked - picked[:, ::-1])
    ep_count = lax.axis_size("ep")
    tp_count = lax.axis_size("tp")
    pair_index = lax.axis_index("tp")
    local_experts = expert_gate.shape[0]
    capacity = 2 * max(1, row_count // expert_count)
    total_slots = expert_count * capacity
    own_slots = total_slots // tp_count
    flat_routes = routes.reshape(row_count * top_count)
    onehot = (flat_routes[:, None] == jnp.arange(expert_count, dtype=jnp.int32)[None, :]).astype(
        jnp.int32
    )
    earlier_count = jnp.sum((jnp.cumsum(onehot, axis=0) - onehot) * onehot, axis=1)
    slot_index = flat_routes * capacity + earlier_count
    pick_all = (slot_index[:, None] == jnp.arange(total_slots, dtype=jnp.int32)[None, :]).astype(
        jnp.bfloat16
    )
    pick_mine = lax.dynamic_slice_in_dim(
        pick_all.reshape(row_count * top_count, ep_count, tp_count, local_experts * capacity),
        pair_index,
        1,
        2,
    ).reshape(row_count * top_count, own_slots)
    outgoing = jnp.einsum(
        "rks,rd->sd",
        pick_mine.reshape(row_count, top_count, own_slots),
        hidden,
        preferred_element_type=jnp.float32,
    ).astype(jnp.bfloat16)
    outgoing = outgoing.reshape(ep_count, local_experts, capacity, model_width)
    col_width = model_width // tp_count
    col_start = pair_index * col_width
    late_decay, late_keys, late_values, outgoing = lax.optimization_barrier(
        (decay_rate, key_rows, value_rows, outgoing)
    )
    new_state = (
        late_decay[..., None] * recurrent_state + late_keys[..., None] * late_values[:, :, None, :]
    )
    arrived = lax.all_to_all(outgoing, "ep", split_axis=0, concat_axis=0, tiled=True)
    arrived, new_state = lax.optimization_barrier((arrived, new_state))
    gate_part = jnp.einsum(
        "secd,edf->secf", arrived, expert_gate, preferred_element_type=jnp.float32
    )
    up_part = jnp.einsum("secd,edf->secf", arrived, expert_up, preferred_element_type=jnp.float32)
    activation = (jax.nn.silu(gate_part) * up_part).astype(jnp.bfloat16)
    results = jnp.einsum(
        "secf,efd->secd", activation, expert_down, preferred_element_type=jnp.float32
    ).astype(jnp.bfloat16)
    halves = jnp.transpose(
        results.reshape(ep_count, local_experts * capacity, tp_count, col_width), (0, 2, 1, 3)
    ).reshape(ep_count * tp_count, local_experts * capacity, col_width)
    returned = lax.all_to_all(halves, ("ep", "tp"), split_axis=0, concat_axis=0, tiled=True)
    fetched = jnp.dot(
        pick_all, returned.reshape(total_slots, col_width), preferred_element_type=jnp.float32
    ).reshape(row_count, top_count, col_width)
    routed_sum = jnp.sum(route_weight[..., None] * fetched, axis=1)
    blended = (
        alpha_res * lax.dynamic_slice_in_dim(hidden, col_start, col_width, 1).astype(jnp.float32)
        + routed_sum
    )
    own_stats = jnp.stack((jnp.sum(blended, axis=1), jnp.sum(blended * blended, axis=1)))
    row_total, row_squares = own_stats + swapped(own_stats)
    row_mean = row_total / model_width
    spread = row_squares / model_width - row_mean * row_mean
    gain_part = lax.dynamic_slice_in_dim(norm_gain[1], col_start, col_width, 0)
    shift_part = lax.dynamic_slice_in_dim(norm_bias[1], col_start, col_width, 0)
    new_tokens = (
        (blended - row_mean[:, None]) * lax.rsqrt(spread[:, None] + eps_norm) * gain_part
        + shift_part
    ).astype(jnp.bfloat16)
    return (new_tokens, new_state)


def solution(mesh):
    in_specs = (
        P("ep", None),
        P("ep", "tp", None, None),
        P(None, "tp"),
        P(None, "tp"),
        P(None, "tp"),
        P(None, "tp"),
        P(None, "tp"),
        P(),
        P("tp", None),
        P(),
        P(),
        P(),
        P(),
        P("ep", None),
        P(("ep", "tp"), None, None),
        P(("ep", "tp"), None, None),
        P(("ep", "tp"), None, None),
    )
    out_specs = (P("ep", "tp"), P("ep", "tp", None, None))
    return jax.shard_map(
        on_device, mesh=mesh, in_specs=in_specs, out_specs=out_specs, check_vma=False
    )
```

```python
import functools

import jax
import jax.numpy as jnp
from jax import lax
from jax.experimental import pallas as pl
from jax.experimental.pallas import tpu as pltpu
from jax.sharding import PartitionSpec as P

alpha_res = 2.0**0.5
eps_norm = 1e-05
mib = 1024 * 1024
cells = 8
in_vmem = pl.BlockSpec(memory_space=pltpu.VMEM)
in_hbm = pl.BlockSpec(memory_space=pltpu.HBM)
in_smem = pl.BlockSpec(memory_space=pltpu.SMEM)


def swapped(values):
    count = lax.axis_size("tp")
    return lax.ppermute(values, "tp", [(i, (i + 1) % count) for i in range(count)])


def dot32(left, right):
    return jnp.dot(left, right, preferred_element_type=jnp.float32)


def mix_kernel(
    key_dim, value_dim, tokens_ref, gain_ref, wq, wd, wk, wv, wg, state, wo,
    part_ref, key_ref, decay_ref, value_ref,
    q_buf, d_buf, k_buf, v_buf, g_buf, s_buf, o_buf, read_buf, sems,
):
    pairs = ((wq, q_buf), (wd, d_buf), (wk, k_buf), (state, s_buf), (wv, v_buf), (wg, g_buf), (wo, o_buf))
    copies = [pltpu.make_async_copy(a, b, sems.at[n]) for n, (a, b) in enumerate(pairs)]
    for copy in copies:
        copy.start()
    heads = q_buf.shape[1] // key_dim
    row_count = tokens_ref.shape[0]
    copies[0].wait()
    queries = dot32(tokens_ref[...], q_buf[...]) * key_dim ** (-0.5)
    copies[1].wait()
    raw = dot32(tokens_ref[...], d_buf[...])
    log_sig = jnp.minimum(raw, 0.0) - jnp.log(1.0 + jnp.exp(-jnp.abs(raw)))
    decay = jnp.exp(log_sig / 16.0)
    decay_ref[...] = decay
    copies[2].wait()
    keys = dot32(tokens_ref[...], k_buf[...])
    key_ref[...] = keys
    scaled = queries * decay
    copies[3].wait()
    for h in range(heads):
        cols = jnp.transpose(scaled[:, h * key_dim : (h + 1) * key_dim])
        for b in range(row_count):
            read_buf[h, b : b + 1, :] = jnp.sum(
                cols[:, b : b + 1] * s_buf[b, h], axis=0, keepdims=True
            )
    copies[4].wait()
    values = dot32(tokens_ref[...], v_buf[...])
    value_ref[...] = values
    copies[5].wait()
    gates = dot32(tokens_ref[...], g_buf[...])
    gates = gates * jax.nn.sigmoid(gates)
    gated = []
    for h in range(heads):
        ks = slice(h * key_dim, (h + 1) * key_dim)
        vs = slice(h * value_dim, (h + 1) * value_dim)
        readout = read_buf[h] + jnp.sum(queries[:, ks] * keys[:, ks], axis=1, keepdims=True) * values[:, vs]
        scale = lax.rsqrt(jnp.mean(readout * readout, axis=1, keepdims=True) + eps_norm)
        gated.append((readout * scale * gain_ref[...] * gates[:, vs]).astype(jnp.bfloat16))
    gated = jnp.concatenate(gated, axis=1)
    copies[6].wait()
    part_ref[...] = dot32(gated, o_buf[...]).astype(jnp.bfloat16)


def mix(tokens, state, wq, wk, wd, wv, wg, gain, wo):
    rows, heads, key_dim, value_dim = state.shape
    f32 = jnp.float32
    weights = (wq, wd, wk, wv, wg)
    return pl.pallas_call(
        functools.partial(mix_kernel, key_dim, value_dim),
        out_shape=(
            jax.ShapeDtypeStruct((rows, wo.shape[1]), jnp.bfloat16),
            jax.ShapeDtypeStruct((rows, wk.shape[1]), f32),
            jax.ShapeDtypeStruct((rows, wd.shape[1]), f32),
            jax.ShapeDtypeStruct((rows, wv.shape[1]), f32),
        ),
        in_specs=[in_vmem] * 2 + [in_hbm] * 7,
        out_specs=[in_vmem] * 4,
        scratch_shapes=[pltpu.VMEM(w.shape, w.dtype) for w in weights]
        + [
            pltpu.VMEM(state.shape, f32),
            pltpu.VMEM(wo.shape, wo.dtype),
            pltpu.VMEM((heads, rows, value_dim), f32),
            pltpu.SemaphoreType.DMA((7,)),
        ],
        compiler_params=pltpu.CompilerParams(vmem_limit_bytes=28 * mib),
        cost_estimate=pl.CostEstimate(flops=200_000_000, bytes_accessed=14 * mib, transcendentals=0),
    )(tokens, gain.reshape(1, -1), wq, wd, wk, wv, wg, state, wo)


def send_kernel(
    tp_count, pieces, pair_ref, own_ref, other_ref, tokens_ref, gain_ref, bias_ref, routes_ref, lanes_ref,
    hidden_ref, out_ref,
):
    mixed = own_ref[...].astype(jnp.float32) + other_ref[...].astype(jnp.float32)
    total = alpha_res * tokens_ref[...].astype(jnp.float32) + mixed
    centered = total - jnp.mean(total, axis=1, keepdims=True)
    spread = jnp.mean(centered * centered, axis=1, keepdims=True)
    hidden = (centered * lax.rsqrt(spread + eps_norm) * gain_ref[0:1, :] + bias_ref[0:1, :]).astype(jnp.bfloat16)
    hidden_ref[...] = hidden
    rows, width = hidden.shape
    span = width // pieces
    lanes = rows * pieces
    top = routes_ref.shape[1]
    cap = cells // pieces
    lane = lax.broadcasted_iota(jnp.int32, (rows, lanes), 1)
    earlier = lax.broadcasted_iota(jnp.int32, (rows, lanes), 0) < lax.rem(lane, rows)
    piece = lax.div(lax.broadcasted_iota(jnp.int32, (1, lanes), 1), rows)
    place = lax.broadcasted_iota(jnp.int32, (out_ref.shape[0], lanes), 0)
    pick = jnp.zeros((out_ref.shape[0], lanes), jnp.float32)
    for k in range(top):
        mine = lanes_ref[k : k + 1, :]
        count = jnp.zeros((1, lanes), jnp.int32)
        for j in range(top):
            same = (routes_ref[:, j : j + 1] == mine) & earlier
            count = count + jnp.sum(same.astype(jnp.int32), axis=0, keepdims=True)
        target = lax.div(mine, tp_count) * cells + count * pieces + piece
        target = jnp.where(lax.rem(mine, tp_count) == pair_ref[0], target, -1)
        pick = pick + (place == target).astype(jnp.float32)
    stack = jnp.concatenate([hidden[:, q * span : (q + 1) * span] for q in range(pieces)], axis=0)
    out_ref[...] = dot32(pick.astype(jnp.bfloat16), stack).astype(jnp.bfloat16)


def expert_kernel(tp_count, pieces, in_ref, gate_ref, up_ref, down_ref, out_ref):
    cap = cells // pieces
    span = in_ref.shape[1]
    total = in_ref.shape[0]
    batch = min(total, 16 * cells)
    sources = batch // cells
    rows = sources * cap
    width = down_ref.shape[2]
    slots = tp_count * pieces
    narrow = width // slots
    row = lax.broadcasted_iota(jnp.int32, (rows, batch), 0)
    col = lax.broadcasted_iota(jnp.int32, (rows, batch), 1)
    place = lax.broadcasted_iota(jnp.int32, (rows * slots, rows * slots), 0)
    origin = lax.broadcasted_iota(jnp.int32, (rows * slots, rows * slots), 1)
    dest = lax.div(place, cells)
    cell = lax.rem(place, cells)
    wanted = (
        (lax.rem(dest, tp_count) * pieces + lax.rem(cell, pieces)) * rows
        + lax.div(dest, tp_count) * cap
        + lax.div(cell, pieces)
    )
    order = (wanted == origin).astype(jnp.float32).astype(jnp.bfloat16)
    for n in range(total // batch):
        block = in_ref[n * batch : (n + 1) * batch, :]
        parts = [
            dot32((col == row * pieces + q).astype(jnp.float32).astype(jnp.bfloat16), block).astype(jnp.bfloat16)
            for q in range(pieces)
        ]
        wide = jnp.concatenate(parts, axis=1)
        gate = dot32(wide, gate_ref[0])
        up = dot32(wide, up_ref[0])
        active = (gate * jax.nn.sigmoid(gate) * up).astype(jnp.bfloat16)
        result = dot32(active, down_ref[0]).astype(jnp.bfloat16)
        stack = jnp.concatenate([result[:, j * narrow : (j + 1) * narrow] for j in range(slots)], axis=0)
        out_ref[n * rows * slots : (n + 1) * rows * slots, :] = dot32(order, stack).astype(jnp.bfloat16)


def blend_kernel(pieces, pair_ref, got_ref, routes_ref, lanes_ref, weight_ref, hidden_ref, blend_ref, stat_ref):
    rows, top = routes_ref.shape
    width = blend_ref.shape[1]
    narrow = got_ref.shape[1]
    cap = cells // pieces
    earlier = lax.broadcasted_iota(jnp.int32, (rows, rows), 1) < lax.broadcasted_iota(jnp.int32, (rows, rows), 0)
    place = lax.broadcasted_iota(jnp.int32, (rows, got_ref.shape[0]), 1)
    picks = []
    for k in range(top):
        mine = routes_ref[:, k : k + 1]
        count = jnp.zeros((rows, 1), jnp.int32)
        for j in range(top):
            same = (lanes_ref[j : j + 1, :rows] == mine) & earlier
            count = count + jnp.sum(same.astype(jnp.int32), axis=1, keepdims=True)
        for q in range(pieces):
            picks.append((place == mine * cells + count * pieces + q).astype(jnp.float32))
    chosen = dot32(jnp.concatenate(picks, axis=0).astype(jnp.bfloat16), got_ref[...])
    start = pl.multiple_of(pair_ref[0] * width, width)
    own = hidden_ref[:, pl.ds(start, width)].astype(jnp.float32)
    total = jnp.zeros((rows, 1), jnp.float32)
    squares = jnp.zeros((rows, 1), jnp.float32)
    for q in range(pieces):
        piece = alpha_res * own[:, q * narrow : (q + 1) * narrow]
        for k in range(top):
            at = (k * pieces + q) * rows
            piece = piece + weight_ref[:, k : k + 1] * chosen[at : at + rows, :]
        blend_ref[:, q * narrow : (q + 1) * narrow] = piece
        total = total + jnp.sum(piece, axis=1, keepdims=True)
        squares = squares + jnp.sum(piece * piece, axis=1, keepdims=True)
    lane = lax.broadcasted_iota(jnp.int32, stat_ref.shape, 1)
    stat_ref[...] = jnp.where(lane == 0, total, jnp.where(lane == 1, squares, 0.0))


def close_kernel(model_width, pair_ref, blend_ref, own_ref, other_ref, gain_ref, bias_ref, out_ref):
    width = blend_ref.shape[1]
    stats = (own_ref[...] + other_ref[...]) / model_width
    mean = stats[:, 0:1]
    spread = stats[:, 1:2] - mean * mean
    start = pl.multiple_of(pair_ref[0] * width, width)
    gain = gain_ref[1:2, pl.ds(start, width)]
    bias = bias_ref[1:2, pl.ds(start, width)]
    out_ref[...] = ((blend_ref[...] - mean) * lax.rsqrt(spread + eps_norm) * gain + bias).astype(jnp.bfloat16)


def small_call(kernel, shapes, specs, limit, flops):
    return pl.pallas_call(
        kernel,
        out_shape=shapes,
        in_specs=specs,
        out_specs=[in_vmem] * len(shapes),
        compiler_params=pltpu.CompilerParams(vmem_limit_bytes=limit * mib),
        cost_estimate=pl.CostEstimate(flops=flops, bytes_accessed=mib, transcendentals=0),
    )


def on_device(
    tokens,
    recurrent_state,
    query_weight,
    key_weight,
    decay_weight,
    value_weight,
    gate_weight,
    head_gain,
    output_weight,
    norm_gain,
    norm_bias,
    group_router,
    router_weight,
    routes,
    expert_gate,
    expert_up,
    expert_down,
):
    row_count, model_width = tokens.shape
    heads_here = recurrent_state.shape[1]
    key_dim = recurrent_state.shape[2]
    value_dim = recurrent_state.shape[3]

    tp_count = lax.axis_size("tp")
    ep_count = lax.axis_size("ep")
    pair_index = lax.axis_index("tp")
    pair = pair_index.reshape(1).astype(jnp.int32)
    own_part, key_rows, decay_rate, value_rows = mix(
        tokens, recurrent_state, query_weight, key_weight, decay_weight, value_weight, gate_weight,
        head_gain, output_weight,
    )
    capacity = 2 * max(1, row_count // router_weight.shape[1])
    pieces = cells // capacity
    lanes = jnp.tile(routes.T, (1, pieces))
    other_part = swapped(own_part)
    hidden, outgoing = small_call(
        functools.partial(send_kernel, tp_count, pieces),
        (
            jax.ShapeDtypeStruct((row_count, model_width), jnp.bfloat16),
            jax.ShapeDtypeStruct((ep_count * cells, model_width // pieces), jnp.bfloat16),
        ),
        [in_smem] + [in_vmem] * 7,
        8,
        20_000_000,
    )(pair, own_part, other_part, tokens, norm_gain, norm_bias, routes, lanes)
    group_count = group_router.shape[1]
    expert_count = router_weight.shape[1]
    per_group = expert_count // group_count
    top_count = routes.shape[1]
    group_logit = jnp.dot(hidden, group_router, preferred_element_type=jnp.float32)
    expert_logit = jnp.dot(hidden, router_weight, preferred_element_type=jnp.float32)
    chosen_group = routes[:, 0] // per_group
    group_hit = chosen_group[:, None] == jnp.arange(group_count, dtype=jnp.int32)[None, :]
    own_logit = jnp.sum(jnp.where(group_hit, group_logit, 0.0), axis=1, keepdims=True)
    group_share = 1.0 / jnp.sum(jnp.exp(group_logit - own_logit), axis=1)
    expert_hit = routes[:, :, None] == jnp.arange(expert_count, dtype=jnp.int32)[None, None, :]
    picked = jnp.sum(jnp.where(expert_hit, expert_logit[:, None, :], 0.0), axis=2)
    route_weight = group_share[:, None] * jax.nn.sigmoid(picked - picked[:, ::-1])
    late_decay, late_keys, late_values, outgoing = lax.optimization_barrier(
        (decay_rate, key_rows, value_rows, outgoing)
    )
    new_state = (
        late_decay.reshape(row_count, heads_here, key_dim, 1) * recurrent_state
        + late_keys.reshape(row_count, heads_here, key_dim, 1)
        * late_values.reshape(row_count, heads_here, 1, value_dim)
    )
    arrived = lax.all_to_all(
        outgoing.reshape(ep_count, cells, model_width // pieces), "ep", split_axis=0, concat_axis=0, tiled=True
    )
    arrived, new_state = lax.optimization_barrier((arrived, new_state))
    col_width = model_width // tp_count
    narrow = col_width // pieces
    device_count = ep_count * tp_count
    (results,) = small_call(
        functools.partial(expert_kernel, tp_count, pieces),
        (jax.ShapeDtypeStruct((device_count * cells, narrow), jnp.bfloat16),),
        [in_vmem] * 4,
        16,
        100_000_000,
    )(arrived.reshape(ep_count * cells, model_width // pieces), expert_gate, expert_up, expert_down)
    returned = lax.all_to_all(
        results.reshape(device_count, cells, narrow), ("ep", "tp"), split_axis=0, concat_axis=0, tiled=True
    )
    blended, own_stats = small_call(
        functools.partial(blend_kernel, pieces),
        (
            jax.ShapeDtypeStruct((row_count, col_width), jnp.float32),
            jax.ShapeDtypeStruct((row_count, 128), jnp.float32),
        ),
        [in_smem] + [in_vmem] * 5,
        8,
        20_000_000,
    )(pair, returned.reshape(device_count * cells, narrow), routes, lanes, route_weight, hidden)
    other_stats = swapped(own_stats)
    (new_tokens,) = small_call(
        functools.partial(close_kernel, model_width),
        (jax.ShapeDtypeStruct((row_count, col_width), jnp.bfloat16),),
        [in_smem] + [in_vmem] * 5,
        8,
        1_000_000,
    )(pair, blended, own_stats, other_stats, norm_gain, norm_bias)
    return (new_tokens, new_state)


def solution(mesh):
    in_specs = (
        P("ep", None),
        P("ep", "tp", None, None),
        P(None, "tp"),
        P(None, "tp"),
        P(None, "tp"),
        P(None, "tp"),
        P(None, "tp"),
        P(),
        P("tp", None),
        P(),
        P(),
        P(),
        P(),
        P("ep", None),
        P(("ep", "tp"), None, None),
        P(("ep", "tp"), None, None),
        P(("ep", "tp"), None, None),
    )
    out_specs = (P("ep", "tp"), P("ep", "tp", None, None))
    return jax.shard_map(
        on_device, mesh=mesh, in_specs=in_specs, out_specs=out_specs, check_vma=False
    )
```

```python
import functools

import jax
import jax.numpy as jnp
from jax import lax
from jax.experimental import pallas as pl
from jax.experimental.pallas import tpu as pltpu
from jax.sharding import PartitionSpec as P

alpha_res = 2.0**0.5
eps_norm = 1e-05
mib = 1024 * 1024
cells = 8
in_vmem = pl.BlockSpec(memory_space=pltpu.VMEM)
in_hbm = pl.BlockSpec(memory_space=pltpu.HBM)
in_smem = pl.BlockSpec(memory_space=pltpu.SMEM)


def swapped(values):
    count = lax.axis_size("tp")
    return lax.ppermute(values, "tp", [(i, (i + 1) % count) for i in range(count)])


def dot32(left, right):
    return jnp.dot(left, right, preferred_element_type=jnp.float32)


def mix_kernel(
    key_dim, value_dim, tokens_ref, gain_ref, wq, wd, wk, wv, wg, state, wo,
    part_ref, key_ref, decay_ref, value_ref,
    q_buf, d_buf, k_buf, v_buf, g_buf, s_buf, o_buf, read_buf, sems,
):
    pairs = ((wq, q_buf), (wd, d_buf), (wk, k_buf), (state, s_buf), (wv, v_buf), (wg, g_buf), (wo, o_buf))
    copies = [pltpu.make_async_copy(a, b, sems.at[n]) for n, (a, b) in enumerate(pairs)]
    for copy in copies:
        copy.start()
    heads = q_buf.shape[1] // key_dim
    row_count = tokens_ref.shape[0]
    copies[0].wait()
    queries = dot32(tokens_ref[...], q_buf[...]) * key_dim ** (-0.5)
    copies[1].wait()
    raw = dot32(tokens_ref[...], d_buf[...])
    log_sig = jnp.minimum(raw, 0.0) - jnp.log(1.0 + jnp.exp(-jnp.abs(raw)))
    decay = jnp.exp(log_sig / 16.0)
    decay_ref[...] = decay
    copies[2].wait()
    keys = dot32(tokens_ref[...], k_buf[...])
    key_ref[...] = keys
    scaled = queries * decay
    copies[3].wait()
    for h in range(heads):
        cols = jnp.transpose(scaled[:, h * key_dim : (h + 1) * key_dim])
        for b in range(row_count):
            read_buf[h, b : b + 1, :] = jnp.sum(
                cols[:, b : b + 1] * s_buf[b, h], axis=0, keepdims=True
            )
    copies[4].wait()
    values = dot32(tokens_ref[...], v_buf[...])
    value_ref[...] = values
    copies[5].wait()
    gates = dot32(tokens_ref[...], g_buf[...])
    gates = gates * jax.nn.sigmoid(gates)
    gated = []
    for h in range(heads):
        ks = slice(h * key_dim, (h + 1) * key_dim)
        vs = slice(h * value_dim, (h + 1) * value_dim)
        readout = read_buf[h] + jnp.sum(queries[:, ks] * keys[:, ks], axis=1, keepdims=True) * values[:, vs]
        scale = lax.rsqrt(jnp.mean(readout * readout, axis=1, keepdims=True) + eps_norm)
        gated.append((readout * scale * gain_ref[...] * gates[:, vs]).astype(jnp.bfloat16))
    gated = jnp.concatenate(gated, axis=1)
    copies[6].wait()
    part_ref[...] = dot32(gated, o_buf[...]).astype(jnp.bfloat16)


def mix(tokens, state, wq, wk, wd, wv, wg, gain, wo):
    rows, heads, key_dim, value_dim = state.shape
    f32 = jnp.float32
    weights = (wq, wd, wk, wv, wg)
    return pl.pallas_call(
        functools.partial(mix_kernel, key_dim, value_dim),
        out_shape=(
            jax.ShapeDtypeStruct((rows, wo.shape[1]), jnp.bfloat16),
            jax.ShapeDtypeStruct((rows, wk.shape[1]), f32),
            jax.ShapeDtypeStruct((rows, wd.shape[1]), f32),
            jax.ShapeDtypeStruct((rows, wv.shape[1]), f32),
        ),
        in_specs=[in_vmem] * 2 + [in_hbm] * 7,
        out_specs=[in_vmem] * 4,
        scratch_shapes=[pltpu.VMEM(w.shape, w.dtype) for w in weights]
        + [
            pltpu.VMEM(state.shape, f32),
            pltpu.VMEM(wo.shape, wo.dtype),
            pltpu.VMEM((heads, rows, value_dim), f32),
            pltpu.SemaphoreType.DMA((7,)),
        ],
        compiler_params=pltpu.CompilerParams(vmem_limit_bytes=60 * mib),
        cost_estimate=pl.CostEstimate(flops=200_000_000, bytes_accessed=14 * mib, transcendentals=0),
    )(tokens, gain.reshape(1, -1), wq, wd, wk, wv, wg, state, wo)


def send_kernel(
    tp_count, pieces, pair_ref, own_ref, other_ref, tokens_ref, gain_ref, bias_ref, routes_ref, lanes_ref,
    hidden_ref, out_ref,
):
    mixed = own_ref[...].astype(jnp.float32) + other_ref[...].astype(jnp.float32)
    total = alpha_res * tokens_ref[...].astype(jnp.float32) + mixed
    centered = total - jnp.mean(total, axis=1, keepdims=True)
    spread = jnp.mean(centered * centered, axis=1, keepdims=True)
    hidden = (centered * lax.rsqrt(spread + eps_norm) * gain_ref[0:1, :] + bias_ref[0:1, :]).astype(jnp.bfloat16)
    hidden_ref[...] = hidden
    rows, width = hidden.shape
    span = width // pieces
    lanes = rows * pieces
    top = routes_ref.shape[1]
    cap = cells // pieces
    lane = lax.broadcasted_iota(jnp.int32, (rows, lanes), 1)
    earlier = lax.broadcasted_iota(jnp.int32, (rows, lanes), 0) < lax.rem(lane, rows)
    piece = lax.div(lax.broadcasted_iota(jnp.int32, (1, lanes), 1), rows)
    place = lax.broadcasted_iota(jnp.int32, (out_ref.shape[0], lanes), 0)
    pick = jnp.zeros((out_ref.shape[0], lanes), jnp.float32)
    for k in range(top):
        mine = lanes_ref[k : k + 1, :]
        count = jnp.zeros((1, lanes), jnp.int32)
        for j in range(top):
            same = (routes_ref[:, j : j + 1] == mine) & earlier
            count = count + jnp.sum(same.astype(jnp.int32), axis=0, keepdims=True)
        target = lax.div(mine, tp_count) * cells + count * pieces + piece
        target = jnp.where(lax.rem(mine, tp_count) == pair_ref[0], target, -1)
        pick = pick + (place == target).astype(jnp.float32)
    stack = jnp.concatenate([hidden[:, q * span : (q + 1) * span] for q in range(pieces)], axis=0)
    out_ref[...] = dot32(pick.astype(jnp.bfloat16), stack).astype(jnp.bfloat16)


def expert_kernel(tp_count, pieces, in_ref, gate_ref, up_ref, down_ref, out_ref):
    cap = cells // pieces
    span = in_ref.shape[1]
    total = in_ref.shape[0]
    batch = min(total, 16 * cells)
    sources = batch // cells
    rows = sources * cap
    width = down_ref.shape[2]
    slots = tp_count * pieces
    narrow = width // slots
    row = lax.broadcasted_iota(jnp.int32, (rows, batch), 0)
    col = lax.broadcasted_iota(jnp.int32, (rows, batch), 1)
    place = lax.broadcasted_iota(jnp.int32, (rows * slots, rows * slots), 0)
    origin = lax.broadcasted_iota(jnp.int32, (rows * slots, rows * slots), 1)
    dest = lax.div(place, cells)
    cell = lax.rem(place, cells)
    wanted = (
        (lax.rem(dest, tp_count) * pieces + lax.rem(cell, pieces)) * rows
        + lax.div(dest, tp_count) * cap
        + lax.div(cell, pieces)
    )
    order = (wanted == origin).astype(jnp.float32).astype(jnp.bfloat16)
    for n in range(total // batch):
        block = in_ref[n * batch : (n + 1) * batch, :]
        parts = [
            dot32((col == row * pieces + q).astype(jnp.float32).astype(jnp.bfloat16), block).astype(jnp.bfloat16)
            for q in range(pieces)
        ]
        wide = jnp.concatenate(parts, axis=1)
        gate = dot32(wide, gate_ref[0])
        up = dot32(wide, up_ref[0])
        active = (gate * jax.nn.sigmoid(gate) * up).astype(jnp.bfloat16)
        result = dot32(active, down_ref[0]).astype(jnp.bfloat16)
        stack = jnp.concatenate([result[:, j * narrow : (j + 1) * narrow] for j in range(slots)], axis=0)
        out_ref[n * rows * slots : (n + 1) * rows * slots, :] = dot32(order, stack).astype(jnp.bfloat16)


def blend_kernel(pieces, pair_ref, got_ref, routes_ref, lanes_ref, weight_ref, hidden_ref, blend_ref, stat_ref):
    rows, top = routes_ref.shape
    width = blend_ref.shape[1]
    narrow = got_ref.shape[1]
    cap = cells // pieces
    earlier = lax.broadcasted_iota(jnp.int32, (rows, rows), 1) < lax.broadcasted_iota(jnp.int32, (rows, rows), 0)
    place = lax.broadcasted_iota(jnp.int32, (rows, got_ref.shape[0]), 1)
    picks = []
    for k in range(top):
        mine = routes_ref[:, k : k + 1]
        count = jnp.zeros((rows, 1), jnp.int32)
        for j in range(top):
            same = (lanes_ref[j : j + 1, :rows] == mine) & earlier
            count = count + jnp.sum(same.astype(jnp.int32), axis=1, keepdims=True)
        for q in range(pieces):
            picks.append((place == mine * cells + count * pieces + q).astype(jnp.float32))
    chosen = dot32(jnp.concatenate(picks, axis=0).astype(jnp.bfloat16), got_ref[...])
    start = pl.multiple_of(pair_ref[0] * width, width)
    own = hidden_ref[:, pl.ds(start, width)].astype(jnp.float32)
    total = jnp.zeros((rows, 1), jnp.float32)
    squares = jnp.zeros((rows, 1), jnp.float32)
    for q in range(pieces):
        piece = alpha_res * own[:, q * narrow : (q + 1) * narrow]
        for k in range(top):
            at = (k * pieces + q) * rows
            piece = piece + weight_ref[:, k : k + 1] * chosen[at : at + rows, :]
        blend_ref[:, q * narrow : (q + 1) * narrow] = piece
        total = total + jnp.sum(piece, axis=1, keepdims=True)
        squares = squares + jnp.sum(piece * piece, axis=1, keepdims=True)
    lane = lax.broadcasted_iota(jnp.int32, stat_ref.shape, 1)
    stat_ref[...] = jnp.where(lane == 0, total, jnp.where(lane == 1, squares, 0.0))


def close_kernel(model_width, pair_ref, blend_ref, own_ref, other_ref, gain_ref, bias_ref, out_ref):
    width = blend_ref.shape[1]
    stats = (own_ref[...] + other_ref[...]) / model_width
    mean = stats[:, 0:1]
    spread = stats[:, 1:2] - mean * mean
    start = pl.multiple_of(pair_ref[0] * width, width)
    gain = gain_ref[1:2, pl.ds(start, width)]
    bias = bias_ref[1:2, pl.ds(start, width)]
    out_ref[...] = ((blend_ref[...] - mean) * lax.rsqrt(spread + eps_norm) * gain + bias).astype(jnp.bfloat16)


def small_call(kernel, shapes, specs, limit, flops):
    return pl.pallas_call(
        kernel,
        out_shape=shapes,
        in_specs=specs,
        out_specs=[in_vmem] * len(shapes),
        compiler_params=pltpu.CompilerParams(vmem_limit_bytes=limit * mib),
        cost_estimate=pl.CostEstimate(flops=flops, bytes_accessed=mib, transcendentals=0),
    )


def on_device(
    tokens,
    recurrent_state,
    query_weight,
    key_weight,
    decay_weight,
    value_weight,
    gate_weight,
    head_gain,
    output_weight,
    norm_gain,
    norm_bias,
    group_router,
    router_weight,
    routes,
    expert_gate,
    expert_up,
    expert_down,
):
    row_count, model_width = tokens.shape
    heads_here = recurrent_state.shape[1]
    key_dim = recurrent_state.shape[2]
    value_dim = recurrent_state.shape[3]

    tp_count = lax.axis_size("tp")
    ep_count = lax.axis_size("ep")
    pair_index = lax.axis_index("tp")
    pair = pair_index.reshape(1).astype(jnp.int32)
    own_part, key_rows, decay_rate, value_rows = mix(
        tokens, recurrent_state, query_weight, key_weight, decay_weight, value_weight, gate_weight,
        head_gain, output_weight,
    )
    capacity = 2 * max(1, row_count // router_weight.shape[1])
    pieces = cells // capacity
    lanes = jnp.tile(routes.T, (1, pieces))
    other_part = swapped(own_part)
    hidden, outgoing = small_call(
        functools.partial(send_kernel, tp_count, pieces),
        (
            jax.ShapeDtypeStruct((row_count, model_width), jnp.bfloat16),
            jax.ShapeDtypeStruct((ep_count * cells, model_width // pieces), jnp.bfloat16),
        ),
        [in_smem] + [in_vmem] * 7,
        8,
        20_000_000,
    )(pair, own_part, other_part, tokens, norm_gain, norm_bias, routes, lanes)
    group_count = group_router.shape[1]
    expert_count = router_weight.shape[1]
    per_group = expert_count // group_count
    top_count = routes.shape[1]
    group_logit = jnp.dot(hidden, group_router, preferred_element_type=jnp.float32)
    expert_logit = jnp.dot(hidden, router_weight, preferred_element_type=jnp.float32)
    chosen_group = routes[:, 0] // per_group
    group_hit = chosen_group[:, None] == jnp.arange(group_count, dtype=jnp.int32)[None, :]
    own_logit = jnp.sum(jnp.where(group_hit, group_logit, 0.0), axis=1, keepdims=True)
    group_share = 1.0 / jnp.sum(jnp.exp(group_logit - own_logit), axis=1)
    expert_hit = routes[:, :, None] == jnp.arange(expert_count, dtype=jnp.int32)[None, None, :]
    picked = jnp.sum(jnp.where(expert_hit, expert_logit[:, None, :], 0.0), axis=2)
    route_weight = group_share[:, None] * jax.nn.sigmoid(picked - picked[:, ::-1])
    late_decay, late_keys, late_values, outgoing = lax.optimization_barrier(
        (decay_rate, key_rows, value_rows, outgoing)
    )
    new_state = (
        late_decay.reshape(row_count, heads_here, key_dim, 1) * recurrent_state
        + late_keys.reshape(row_count, heads_here, key_dim, 1)
        * late_values.reshape(row_count, heads_here, 1, value_dim)
    )
    arrived = lax.all_to_all(
        outgoing.reshape(ep_count, cells, model_width // pieces), "ep", split_axis=0, concat_axis=0, tiled=True
    )
    arrived, new_state = lax.optimization_barrier((arrived, new_state))
    col_width = model_width // tp_count
    narrow = col_width // pieces
    device_count = ep_count * tp_count
    (results,) = small_call(
        functools.partial(expert_kernel, tp_count, pieces),
        (jax.ShapeDtypeStruct((device_count * cells, narrow), jnp.bfloat16),),
        [in_vmem] * 4,
        16,
        100_000_000,
    )(arrived.reshape(ep_count * cells, model_width // pieces), expert_gate, expert_up, expert_down)
    returned = lax.all_to_all(
        results.reshape(device_count, cells, narrow), ("ep", "tp"), split_axis=0, concat_axis=0, tiled=True
    )
    blended, own_stats = small_call(
        functools.partial(blend_kernel, pieces),
        (
            jax.ShapeDtypeStruct((row_count, col_width), jnp.float32),
            jax.ShapeDtypeStruct((row_count, 128), jnp.float32),
        ),
        [in_smem] + [in_vmem] * 5,
        8,
        20_000_000,
    )(pair, returned.reshape(device_count * cells, narrow), routes, lanes, route_weight, hidden)
    other_stats = swapped(own_stats)
    (new_tokens,) = small_call(
        functools.partial(close_kernel, model_width),
        (jax.ShapeDtypeStruct((row_count, col_width), jnp.bfloat16),),
        [in_smem] + [in_vmem] * 5,
        8,
        1_000_000,
    )(pair, blended, own_stats, other_stats, norm_gain, norm_bias)
    return (new_tokens, new_state)


def solution(mesh):
    in_specs = (
        P("ep", None),
        P("ep", "tp", None, None),
        P(None, "tp"),
        P(None, "tp"),
        P(None, "tp"),
        P(None, "tp"),
        P(None, "tp"),
        P(),
        P("tp", None),
        P(),
        P(),
        P(),
        P(),
        P("ep", None),
        P(("ep", "tp"), None, None),
        P(("ep", "tp"), None, None),
        P(("ep", "tp"), None, None),
    )
    out_specs = (P("ep", "tp"), P("ep", "tp", None, None))
    return jax.shard_map(
        on_device, mesh=mesh, in_specs=in_specs, out_specs=out_specs, check_vma=False
    )
```

```python
import functools

import jax
import jax.numpy as jnp
from jax import lax
from jax.experimental import pallas as pl
from jax.experimental.pallas import tpu as pltpu
from jax.sharding import PartitionSpec as P

alpha_res = 2.0**0.5
eps_norm = 1e-05
mib = 1024 * 1024
cells = 8
in_vmem = pl.BlockSpec(memory_space=pltpu.VMEM)
in_hbm = pl.BlockSpec(memory_space=pltpu.HBM)
in_smem = pl.BlockSpec(memory_space=pltpu.SMEM)


def swapped(values):
    count = lax.axis_size("tp")
    return lax.ppermute(values, "tp", [(i, (i + 1) % count) for i in range(count)])


def dot32(left, right):
    return jnp.dot(left, right, preferred_element_type=jnp.float32)


def mix_kernel(
    key_dim, value_dim, tokens_ref, gain_ref, wq, wd, wk, wv, wg, state, wo,
    part_ref, key_ref, decay_ref, value_ref,
    q_buf, d_buf, k_buf, v_buf, g_buf, s_buf, o_buf, read_buf, sems,
):
    pairs = ((wq, q_buf), (wd, d_buf), (wk, k_buf), (state, s_buf), (wv, v_buf), (wg, g_buf), (wo, o_buf))
    copies = [pltpu.make_async_copy(a, b, sems.at[n]) for n, (a, b) in enumerate(pairs)]
    for copy in copies:
        copy.start()
    heads = q_buf.shape[1] // key_dim
    row_count = tokens_ref.shape[0]
    copies[0].wait()
    queries = dot32(tokens_ref[...], q_buf[...]) * key_dim ** (-0.5)
    copies[1].wait()
    raw = dot32(tokens_ref[...], d_buf[...])
    log_sig = jnp.minimum(raw, 0.0) - jnp.log(1.0 + jnp.exp(-jnp.abs(raw)))
    decay = jnp.exp(log_sig / 16.0)
    for h in range(heads):
        decay_ref[:, h, :] = decay[:, h * key_dim : (h + 1) * key_dim]
    copies[2].wait()
    keys = dot32(tokens_ref[...], k_buf[...])
    for h in range(heads):
        key_ref[:, h, :] = keys[:, h * key_dim : (h + 1) * key_dim]
    scaled = queries * decay
    copies[3].wait()
    for h in range(heads):
        cols = jnp.transpose(scaled[:, h * key_dim : (h + 1) * key_dim])
        for b in range(row_count):
            read_buf[h, b : b + 1, :] = jnp.sum(
                cols[:, b : b + 1] * s_buf[b, h], axis=0, keepdims=True
            )
    copies[4].wait()
    values = dot32(tokens_ref[...], v_buf[...])
    for h in range(heads):
        value_ref[:, h, :] = values[:, h * value_dim : (h + 1) * value_dim]
    copies[5].wait()
    gates = dot32(tokens_ref[...], g_buf[...])
    gates = gates * jax.nn.sigmoid(gates)
    gated = []
    for h in range(heads):
        ks = slice(h * key_dim, (h + 1) * key_dim)
        vs = slice(h * value_dim, (h + 1) * value_dim)
        readout = read_buf[h] + jnp.sum(queries[:, ks] * keys[:, ks], axis=1, keepdims=True) * values[:, vs]
        scale = lax.rsqrt(jnp.mean(readout * readout, axis=1, keepdims=True) + eps_norm)
        gated.append((readout * scale * gain_ref[...] * gates[:, vs]).astype(jnp.bfloat16))
    gated = jnp.concatenate(gated, axis=1)
    copies[6].wait()
    part_ref[...] = dot32(gated, o_buf[...]).astype(jnp.bfloat16)


def mix(tokens, state, wq, wk, wd, wv, wg, gain, wo):
    rows, heads, key_dim, value_dim = state.shape
    f32 = jnp.float32
    weights = (wq, wd, wk, wv, wg)
    return pl.pallas_call(
        functools.partial(mix_kernel, key_dim, value_dim),
        out_shape=(
            jax.ShapeDtypeStruct((rows, wo.shape[1]), jnp.bfloat16),
            jax.ShapeDtypeStruct((rows, heads, key_dim), f32),
            jax.ShapeDtypeStruct((rows, heads, key_dim), f32),
            jax.ShapeDtypeStruct((rows, heads, value_dim), f32),
        ),
        in_specs=[in_vmem] * 2 + [in_hbm] * 7,
        out_specs=[in_vmem] * 4,
        scratch_shapes=[pltpu.VMEM(w.shape, w.dtype) for w in weights]
        + [
            pltpu.VMEM(state.shape, f32),
            pltpu.VMEM(wo.shape, wo.dtype),
            pltpu.VMEM((heads, rows, value_dim), f32),
            pltpu.SemaphoreType.DMA((7,)),
        ],
        compiler_params=pltpu.CompilerParams(vmem_limit_bytes=53 * mib),
        cost_estimate=pl.CostEstimate(flops=200_000_000, bytes_accessed=14 * mib, transcendentals=0),
    )(tokens, gain.reshape(1, -1), wq, wd, wk, wv, wg, state, wo)


def send_kernel(
    tp_count, pieces, pair_ref, own_ref, other_ref, tokens_ref, gain_ref, bias_ref, routes_ref, lanes_ref,
    hidden_ref, out_ref,
):
    mixed = own_ref[...].astype(jnp.float32) + other_ref[...].astype(jnp.float32)
    total = alpha_res * tokens_ref[...].astype(jnp.float32) + mixed
    centered = total - jnp.mean(total, axis=1, keepdims=True)
    spread = jnp.mean(centered * centered, axis=1, keepdims=True)
    hidden = (centered * lax.rsqrt(spread + eps_norm) * gain_ref[0:1, :] + bias_ref[0:1, :]).astype(jnp.bfloat16)
    hidden_ref[...] = hidden
    rows, width = hidden.shape
    span = width // pieces
    lanes = rows * pieces
    top = routes_ref.shape[1]
    cap = cells // pieces
    lane = lax.broadcasted_iota(jnp.int32, (rows, lanes), 1)
    earlier = lax.broadcasted_iota(jnp.int32, (rows, lanes), 0) < lax.rem(lane, rows)
    piece = lax.div(lax.broadcasted_iota(jnp.int32, (1, lanes), 1), rows)
    place = lax.broadcasted_iota(jnp.int32, (out_ref.shape[0], lanes), 0)
    pick = jnp.zeros((out_ref.shape[0], lanes), jnp.float32)
    for k in range(top):
        mine = lanes_ref[k : k + 1, :]
        count = jnp.zeros((1, lanes), jnp.int32)
        for j in range(top):
            same = (routes_ref[:, j : j + 1] == mine) & earlier
            count = count + jnp.sum(same.astype(jnp.int32), axis=0, keepdims=True)
        target = lax.div(mine, tp_count) * cells + count * pieces + piece
        target = jnp.where(lax.rem(mine, tp_count) == pair_ref[0], target, -1)
        pick = pick + (place == target).astype(jnp.float32)
    stack = jnp.concatenate([hidden[:, q * span : (q + 1) * span] for q in range(pieces)], axis=0)
    out_ref[...] = dot32(pick.astype(jnp.bfloat16), stack).astype(jnp.bfloat16)


def expert_kernel(tp_count, pieces, in_ref, gate_ref, up_ref, down_ref, out_ref):
    cap = cells // pieces
    span = in_ref.shape[1]
    total = in_ref.shape[0]
    batch = min(total, 16 * cells)
    sources = batch // cells
    rows = sources * cap
    width = down_ref.shape[2]
    slots = tp_count * pieces
    narrow = width // slots
    row = lax.broadcasted_iota(jnp.int32, (rows, batch), 0)
    col = lax.broadcasted_iota(jnp.int32, (rows, batch), 1)
    place = lax.broadcasted_iota(jnp.int32, (rows * slots, rows * slots), 0)
    origin = lax.broadcasted_iota(jnp.int32, (rows * slots, rows * slots), 1)
    dest = lax.div(place, cells)
    cell = lax.rem(place, cells)
    wanted = (
        (lax.rem(dest, tp_count) * pieces + lax.rem(cell, pieces)) * rows
        + lax.div(dest, tp_count) * cap
        + lax.div(cell, pieces)
    )
    order = (wanted == origin).astype(jnp.float32).astype(jnp.bfloat16)
    for n in range(total // batch):
        block = in_ref[n * batch : (n + 1) * batch, :]
        parts = [
            dot32((col == row * pieces + q).astype(jnp.float32).astype(jnp.bfloat16), block).astype(jnp.bfloat16)
            for q in range(pieces)
        ]
        wide = jnp.concatenate(parts, axis=1)
        gate = dot32(wide, gate_ref[0])
        up = dot32(wide, up_ref[0])
        active = (gate * jax.nn.sigmoid(gate) * up).astype(jnp.bfloat16)
        result = dot32(active, down_ref[0]).astype(jnp.bfloat16)
        stack = jnp.concatenate([result[:, j * narrow : (j + 1) * narrow] for j in range(slots)], axis=0)
        out_ref[n * rows * slots : (n + 1) * rows * slots, :] = dot32(order, stack).astype(jnp.bfloat16)


def blend_kernel(pieces, pair_ref, got_ref, routes_ref, lanes_ref, weight_ref, hidden_ref, blend_ref, stat_ref):
    rows, top = routes_ref.shape
    width = blend_ref.shape[1]
    narrow = got_ref.shape[1]
    cap = cells // pieces
    earlier = lax.broadcasted_iota(jnp.int32, (rows, rows), 1) < lax.broadcasted_iota(jnp.int32, (rows, rows), 0)
    place = lax.broadcasted_iota(jnp.int32, (rows, got_ref.shape[0]), 1)
    picks = []
    for k in range(top):
        mine = routes_ref[:, k : k + 1]
        count = jnp.zeros((rows, 1), jnp.int32)
        for j in range(top):
            same = (lanes_ref[j : j + 1, :rows] == mine) & earlier
            count = count + jnp.sum(same.astype(jnp.int32), axis=1, keepdims=True)
        for q in range(pieces):
            picks.append((place == mine * cells + count * pieces + q).astype(jnp.float32))
    chosen = dot32(jnp.concatenate(picks, axis=0).astype(jnp.bfloat16), got_ref[...])
    start = pl.multiple_of(pair_ref[0] * width, width)
    own = hidden_ref[:, pl.ds(start, width)].astype(jnp.float32)
    total = jnp.zeros((rows, 1), jnp.float32)
    squares = jnp.zeros((rows, 1), jnp.float32)
    for q in range(pieces):
        piece = alpha_res * own[:, q * narrow : (q + 1) * narrow]
        for k in range(top):
            at = (k * pieces + q) * rows
            piece = piece + weight_ref[:, k : k + 1] * chosen[at : at + rows, :]
        blend_ref[:, q * narrow : (q + 1) * narrow] = piece
        total = total + jnp.sum(piece, axis=1, keepdims=True)
        squares = squares + jnp.sum(piece * piece, axis=1, keepdims=True)
    lane = lax.broadcasted_iota(jnp.int32, stat_ref.shape, 1)
    stat_ref[...] = jnp.where(lane == 0, total, jnp.where(lane == 1, squares, 0.0))


def close_kernel(model_width, pair_ref, blend_ref, own_ref, other_ref, gain_ref, bias_ref, out_ref):
    width = blend_ref.shape[1]
    stats = (own_ref[...] + other_ref[...]) / model_width
    mean = stats[:, 0:1]
    spread = stats[:, 1:2] - mean * mean
    start = pl.multiple_of(pair_ref[0] * width, width)
    gain = gain_ref[1:2, pl.ds(start, width)]
    bias = bias_ref[1:2, pl.ds(start, width)]
    out_ref[...] = ((blend_ref[...] - mean) * lax.rsqrt(spread + eps_norm) * gain + bias).astype(jnp.bfloat16)


def small_call(kernel, shapes, specs, limit, flops):
    return pl.pallas_call(
        kernel,
        out_shape=shapes,
        in_specs=specs,
        out_specs=[in_vmem] * len(shapes),
        compiler_params=pltpu.CompilerParams(vmem_limit_bytes=limit * mib),
        cost_estimate=pl.CostEstimate(flops=flops, bytes_accessed=mib, transcendentals=0),
    )


def on_device(
    tokens,
    recurrent_state,
    query_weight,
    key_weight,
    decay_weight,
    value_weight,
    gate_weight,
    head_gain,
    output_weight,
    norm_gain,
    norm_bias,
    group_router,
    router_weight,
    routes,
    expert_gate,
    expert_up,
    expert_down,
):
    row_count, model_width = tokens.shape
    heads_here = recurrent_state.shape[1]
    key_dim = recurrent_state.shape[2]
    value_dim = recurrent_state.shape[3]

    tp_count = lax.axis_size("tp")
    ep_count = lax.axis_size("ep")
    pair_index = lax.axis_index("tp")
    pair = pair_index.reshape(1).astype(jnp.int32)
    own_part, key_rows, decay_rate, value_rows = mix(
        tokens, recurrent_state, query_weight, key_weight, decay_weight, value_weight, gate_weight,
        head_gain, output_weight,
    )
    capacity = 2 * max(1, row_count // router_weight.shape[1])
    pieces = cells // capacity
    lanes = jnp.tile(routes.T, (1, pieces))
    other_part = swapped(own_part)
    hidden, outgoing = small_call(
        functools.partial(send_kernel, tp_count, pieces),
        (
            jax.ShapeDtypeStruct((row_count, model_width), jnp.bfloat16),
            jax.ShapeDtypeStruct((ep_count * cells, model_width // pieces), jnp.bfloat16),
        ),
        [in_smem] + [in_vmem] * 7,
        8,
        20_000_000,
    )(pair, own_part, other_part, tokens, norm_gain, norm_bias, routes, lanes)
    group_count = group_router.shape[1]
    expert_count = router_weight.shape[1]
    per_group = expert_count // group_count
    top_count = routes.shape[1]
    group_logit = jnp.dot(hidden, group_router, preferred_element_type=jnp.float32)
    expert_logit = jnp.dot(hidden, router_weight, preferred_element_type=jnp.float32)
    chosen_group = routes[:, 0] // per_group
    group_hit = chosen_group[:, None] == jnp.arange(group_count, dtype=jnp.int32)[None, :]
    own_logit = jnp.sum(jnp.where(group_hit, group_logit, 0.0), axis=1, keepdims=True)
    group_share = 1.0 / jnp.sum(jnp.exp(group_logit - own_logit), axis=1)
    expert_hit = routes[:, :, None] == jnp.arange(expert_count, dtype=jnp.int32)[None, None, :]
    picked = jnp.sum(jnp.where(expert_hit, expert_logit[:, None, :], 0.0), axis=2)
    route_weight = group_share[:, None] * jax.nn.sigmoid(picked - picked[:, ::-1])
    late_decay, late_keys, late_values, outgoing = lax.optimization_barrier(
        (decay_rate, key_rows, value_rows, outgoing)
    )
    new_state = (
        late_decay[..., None] * recurrent_state
        + late_keys[..., None]
        * late_values[:, :, None, :]
    )
    arrived = lax.all_to_all(
        outgoing.reshape(ep_count, cells, model_width // pieces), "ep", split_axis=0, concat_axis=0, tiled=True
    )
    arrived, new_state = lax.optimization_barrier((arrived, new_state))
    col_width = model_width // tp_count
    narrow = col_width // pieces
    device_count = ep_count * tp_count
    (results,) = small_call(
        functools.partial(expert_kernel, tp_count, pieces),
        (jax.ShapeDtypeStruct((device_count * cells, narrow), jnp.bfloat16),),
        [in_vmem] * 4,
        16,
        100_000_000,
    )(arrived.reshape(ep_count * cells, model_width // pieces), expert_gate, expert_up, expert_down)
    returned = lax.all_to_all(
        results.reshape(device_count, cells, narrow), ("ep", "tp"), split_axis=0, concat_axis=0, tiled=True
    )
    blended, own_stats = small_call(
        functools.partial(blend_kernel, pieces),
        (
            jax.ShapeDtypeStruct((row_count, col_width), jnp.float32),
            jax.ShapeDtypeStruct((row_count, 128), jnp.float32),
        ),
        [in_smem] + [in_vmem] * 5,
        8,
        20_000_000,
    )(pair, returned.reshape(device_count * cells, narrow), routes, lanes, route_weight, hidden)
    other_stats = swapped(own_stats)
    (new_tokens,) = small_call(
        functools.partial(close_kernel, model_width),
        (jax.ShapeDtypeStruct((row_count, col_width), jnp.bfloat16),),
        [in_smem] + [in_vmem] * 5,
        8,
        1_000_000,
    )(pair, blended, own_stats, other_stats, norm_gain, norm_bias)
    return (new_tokens, new_state)


def solution(mesh):
    in_specs = (
        P("ep", None),
        P("ep", "tp", None, None),
        P(None, "tp"),
        P(None, "tp"),
        P(None, "tp"),
        P(None, "tp"),
        P(None, "tp"),
        P(),
        P("tp", None),
        P(),
        P(),
        P(),
        P(),
        P("ep", None),
        P(("ep", "tp"), None, None),
        P(("ep", "tp"), None, None),
        P(("ep", "tp"), None, None),
    )
    out_specs = (P("ep", "tp"), P("ep", "tp", None, None))
    return jax.shard_map(
        on_device, mesh=mesh, in_specs=in_specs, out_specs=out_specs, check_vma=False
    )
```
